32 devices in a mesh: grp: 2 (over y), dp: 2 (over x), kv: 4 (over z), tp: 2 (over core).
Axes of the slice: x: 2, y: 2, z: 4, core: 2. Of those that a mesh axis runs over, the one named last changes fastest.
Arguments:
- tokens: bfloat16 [96, 4, 4096], P(('grp', 'dp'), None, ('kv', 'tp')), parts along dimension 0, may hold values from -6 to 6
- norm_gain: float32 [4096], replicated, may hold values from 0.1 to 1.9
- w_query: bfloat16 [16, 128, 4096], P('kv', 'tp'), may hold values from -0.09375 to 0.09375
- w_key: bfloat16 [16, 128, 4096], P('kv', 'tp'), may hold values from -0.09375 to 0.09375
- w_value: bfloat16 [16, 128, 4096], P('kv', 'tp'), may hold values from -0.09375 to 0.09375
- w_gate: bfloat16 [16, 128, 4096], P('kv', 'tp'), may hold values from -0.09375 to 0.09375
- w_decay: bfloat16 [4096, 16], replicated, may hold values from -0.09375 to 0.09375
- w_beta: bfloat16 [4096, 16], replicated, may hold values from -0.09375 to 0.09375
- decay_rate: float32 [16], P('kv'), may hold values from 0.02 to 1
- head_gain: float32 [128], P('tp'), may hold values from 0.1 to 1.9
- w_out: bfloat16 [16, 128, 4096], P('kv', 'tp'), may hold values from -0.1875 to 0.1875
- state: float32 [96, 16, 128, 128], P(('grp', 'dp'), 'kv', 'tp'), parts along dimension 0, may hold values from -6 to 6
- prev_keys: bfloat16 [96, 4, 16, 128], P(('grp', 'dp'), None, 'kv'), parts along dimension 0, may hold values from -6 to 6
- prev_values: bfloat16 [96, 4, 16, 128], P(('grp', 'dp'), None, 'kv', 'tp'), parts along dimension 0, may hold values from -6 to 6
- prev_decay: float32 [96, 4, 16], P(('grp', 'dp'), None, 'kv'), parts along dimension 0, may hold values from 0.01 to 1
- prev_beta: float32 [96, 4, 16], P(('grp', 'dp'), None, 'kv'), parts along dimension 0, may hold values from 0.05 to 1
- accepted: int32 [96], P(('grp', 'dp')), parts along dimension 0, may hold values from 0 to 4
Outputs:
- mixed: bfloat16 [96, 4, 4096], P(('grp', 'dp'), None, ('kv', 'tp')), parts along dimension 0
- committed: float32 [96, 16, 128, 128], P(('grp', 'dp'), 'kv', 'tp'), parts along dimension 0
The draws below stay inside these ranges and needn't reach their ends.
There are 2 independent parts, one for each index of `grp`. The reference program is written for one: setup_inputs(seed, part) draws one part's arguments, and reference() takes and returns one part's arrays. A program takes and returns all parts, laid end to end along the dimension named above; an argument that names none is the same for every part. Nothing has to cross between parts.
All inputs are finite; a program needn't handle non-finite values.
Results may differ from the reference program's by a relative error of at most 0.015.
Values may be sent and summed in bfloat16 or wider, within the bound.
A program may use at most 64 MiB of HBM per device.

```python
import math
import jax
import jax.numpy as jnp
from jax import lax

D = 4096
H = 16
DK = 128
DV = 128
P_SIZE = 4
SEQS = 48


def touch_ends(drawn, own_key, least, largest):
    extent = drawn.shape
    spot = [jax.random.randint(jax.random.fold_in(own_key, axis), (), 0, extent[axis]) for axis in range(len(extent))]
    drawn = drawn.at[tuple(spot)].set(least)
    longest = extent.index(max(extent))
    spot[longest] = (spot[longest] + 1) % extent[longest]
    return drawn.at[tuple(spot)].set(largest)


def with_spikes(drawn, own_key, source, target, parts, factor):
    owner, partner = [(jnp.arange(drawn.shape[axis_at]) // (drawn.shape[axis_at] // parts)).reshape([-1 if axis == axis_at else 1 for axis in range(drawn.ndim)]) for axis_at in (source, target)]
    chosen = jax.random.permutation(own_key, parts)[partner]
    strong = (owner == chosen) | (owner == (partner + parts // 2) % parts)
    return jnp.where(strong, factor * drawn, drawn)


def shard_levels(own_key, dims, shards, least, top_value):
    loudness, own = 1.0, jax.random.fold_in(own_key, 6)
    for axis_at, blocks in shards:
        steps = jnp.exp(jax.random.uniform(jax.random.fold_in(own, axis_at), (blocks,), jnp.float32, least / len(shards), top_value / len(shards)))
        loudness = loudness * jnp.repeat(steps, dims[axis_at] // blocks).reshape([-1 if axis == axis_at else 1 for axis in range(len(dims))])
    return loudness


def gaussian(rng, shape, deviation, bound, split=(), held_as=jnp.bfloat16):
    loudness = shard_levels(rng, shape, split, -0.22, 0.18) if split else 1.0
    drawn = jax.random.normal(rng, shape, jnp.float32) * deviation * loudness
    return jnp.minimum(jnp.maximum(drawn, -bound), bound).astype(held_as)


def heavy_noise(key, dims, width, bound, split, heavy, kind=jnp.bfloat16):
    array = width * jax.random.normal(key, dims, jnp.float32)
    if split:
        array = array * shard_levels(key, dims, split, -0.22, 0.18)
    return jnp.clip(with_spikes(array, jax.random.fold_in(key, 3), *heavy), -bound, bound).astype(kind)


def setup_inputs(seed: int = 0, part: int = 0) -> dict:
    streams_of = jax.random.split(jax.random.key(seed), 18)
    part_keys = jax.random.split(jax.random.fold_in(streams_of[17], part), 18)
    return {
        "tokens": gaussian(part_keys[0], (SEQS, P_SIZE, D), 1.0, 6.0, ((0, 2), (2, 8))),
        "norm_gain": jnp.clip(1.0 + 0.18 * jax.random.normal(streams_of[1], (D,), jnp.float32), 0.1, 1.9),
        "w_query": gaussian(streams_of[2], (H, DK, D), D ** -0.5, 0.09375, ((0, 4), (1, 2))),
        "w_key": gaussian(streams_of[3], (H, DK, D), D ** -0.5, 0.09375, ((0, 4), (1, 2))),
        "w_value": gaussian(streams_of[4], (H, DV, D), D ** -0.5, 0.09375, ((0, 4), (1, 2))),
        "w_gate": gaussian(streams_of[5], (H, DV, D), D ** -0.5, 0.09375, ((0, 4), (1, 2))),
        "w_decay": gaussian(streams_of[6], (D, H), D ** -0.5, 0.09375),
        "w_beta": gaussian(streams_of[7], (D, H), D ** -0.5, 0.09375),
        "decay_rate": jnp.clip(jnp.exp(math.log(1.0) - 3.912023 * jax.random.uniform(streams_of[8], (H,), jnp.float32) ** shard_levels(streams_of[8], (H,), ((0, 4),), -0.2, 0.2)), 0.02, 1.0),
        "head_gain": jnp.clip(1.0 + 0.18 * jax.random.normal(streams_of[9], (DV,), jnp.float32), 0.1, 1.9),
        "w_out": heavy_noise(streams_of[10], (H, DV, D), (H * DV) ** -0.5, 0.1875, ((0, 4), (1, 2)), (0, 2, 4, 2.0)),
        "state": gaussian(part_keys[11], (SEQS, H, DV, DK), 1.0, 6.0, ((0, 2), (1, 4), (2, 2)), jnp.float32),
        "prev_keys": gaussian(part_keys[12], (SEQS, P_SIZE, H, DK), 1.0, 6.0, ((0, 2), (2, 4))),
        "prev_values": gaussian(part_keys[13], (SEQS, P_SIZE, H, DV), 1.0, 6.0, ((0, 2), (2, 4), (3, 2))),
        "prev_decay": jnp.clip(jnp.exp(math.log(1.0) - 4.6051702 * jax.random.uniform(part_keys[14], (SEQS, P_SIZE, H), jnp.float32) ** shard_levels(part_keys[14], (SEQS, P_SIZE, H), ((0, 2), (2, 4)), -0.2, 0.2)), 0.01, 1.0),
        "prev_beta": jnp.clip(0.05 + 0.95 * jax.random.uniform(part_keys[15], (SEQS, P_SIZE, H), jnp.float32) ** shard_levels(part_keys[15], (SEQS, P_SIZE, H), ((0, 2), (2, 4)), -0.2, 0.2), 0.05, 1.0),
        "accepted": touch_ends(jax.random.randint(part_keys[16], (SEQS,), 0, P_SIZE + 1), jax.random.fold_in(part_keys[16], 1), 0, P_SIZE).astype(jnp.int32),
    }


EPS = 1e-06
PRECISE = lax.Precision.HIGHEST

def unit_rows(values):
    return values * lax.rsqrt(lax.optimization_barrier(jnp.sum(values * values, axis=-1, keepdims=True)) + EPS)

def delta_update(carried, keys_now, values_now, retain, strength):
    carried = carried * retain[..., None, None]
    predicted = jnp.einsum('shed,shd->she', carried, keys_now, precision=PRECISE)
    update = strength[..., None] * (values_now - predicted)
    return carried + update[..., :, None] * keys_now[..., None, :]

def reference(tokens, norm_gain, w_query, w_key, w_value, w_gate, w_decay, w_beta, decay_rate, head_gain, w_out, state, prev_keys, prev_values, prev_decay, prev_beta, accepted):
    floats = tokens.astype(jnp.float32)
    normed = (floats * lax.rsqrt(lax.optimization_barrier(jnp.mean(floats * floats, axis=-1, keepdims=True)) + EPS) * norm_gain).astype(jnp.bfloat16)
    flat_rows = normed.reshape(SEQS * P_SIZE, D)

    def project(weight):
        product = lax.dot_general(flat_rows, weight.reshape(-1, D), (((1,), (1,)), ((), ())), preferred_element_type=jnp.float32)
        return product.astype(jnp.bfloat16).reshape(SEQS, P_SIZE, H, -1)
    query = project(w_query)
    key_raw = project(w_key)
    value_raw = project(w_value)
    gate_raw = project(w_gate)
    decay_pre = jnp.dot(flat_rows, w_decay, preferred_element_type=jnp.float32).reshape(SEQS, P_SIZE, H)
    beta_pre = jnp.dot(flat_rows, w_beta, preferred_element_type=jnp.float32).reshape(SEQS, P_SIZE, H)
    forget = decay_rate * jax.nn.softplus(decay_pre)
    strength = jax.nn.sigmoid(beta_pre)
    queries = unit_rows(jax.nn.silu(query.astype(jnp.float32))) * DK ** (-0.5)
    key_unit = unit_rows(jax.nn.silu(key_raw.astype(jnp.float32)))
    value_act = jax.nn.silu(value_raw.astype(jnp.float32))
    old_keys = unit_rows(prev_keys.astype(jnp.float32))
    old_values = prev_values.astype(jnp.float32)
    carried = state
    for position in range(P_SIZE):
        accept_mask = (position < accepted).astype(jnp.float32)[:, None]
        carried = delta_update(carried, old_keys[:, position], old_values[:, position], jnp.exp(-prev_decay[:, position] * accept_mask), prev_beta[:, position] * accept_mask)
    committed = carried
    outputs = []
    for position in range(P_SIZE):
        carried = delta_update(carried, key_unit[:, position], value_act[:, position], jnp.exp(-forget[:, position]), strength[:, position])
        outputs.append(jnp.einsum('shed,shd->she', carried, queries[:, position], precision=PRECISE))
    heads_out = jnp.stack(outputs, axis=1)
    scaled = (heads_out * lax.rsqrt(lax.optimization_barrier(jnp.mean(heads_out * heads_out, axis=-1, keepdims=True)) + EPS) * head_gain * jax.nn.silu(gate_raw.astype(jnp.float32))).astype(jnp.bfloat16)
    mixed_out = jnp.dot(scaled.reshape(SEQS * P_SIZE, H * DV), w_out.reshape(H * DV, D), preferred_element_type=jnp.float32).astype(jnp.bfloat16)
    return (mixed_out.reshape(SEQS, P_SIZE, D), committed)
```

```python
import functools

import jax
import jax.numpy as jnp
from jax import lax
from jax.experimental import pallas as pl
from jax.experimental.pallas import tpu as pltpu
from jax.sharding import PartitionSpec as P

EPS = 1e-06
F32 = jnp.float32
BF16 = jnp.bfloat16
MESH = pl.DeviceIdType.MESH
NT = (((1,), (1,)), ((), ()))
TN = (((0,), (0,)), ((), ()))


def dot_nt(a, b):
    return lax.dot_general(a, b, NT, preferred_element_type=F32)


def silu(u):
    return u * jax.nn.sigmoid(u)


def lane_group(rows, cols, group):
    return lax.broadcasted_iota(jnp.int32, (rows, cols), 1) // group


def block_ones(rows, row_group, cols, col_group):
    r = lax.broadcasted_iota(jnp.int32, (rows, cols), 0) // row_group
    return (r == lane_group(rows, cols, col_group)).astype(F32).astype(BF16)


def put(buf, rows, x):
    cols = x.shape[1]
    if cols < 128:
        x = jnp.concatenate([x] * (128 // cols), axis=1)
    for c in range(buf.shape[0]):
        buf[c, rows, :] = x[:, c * 128 : (c + 1) * 128]


def get(buf, rows, cols):
    x = jnp.concatenate([buf[c, rows, :] for c in range(buf.shape[0])], axis=1)
    return x[:, :cols]


def own_head(parts, group):
    rows, cols = parts[0].shape
    if len(parts) == 1:
        return parts[0]
    lanes = lane_group(rows, cols, group)
    total = jnp.where(lanes == 0, parts[0], 0.0)
    for h in range(1, len(parts)):
        total = jnp.where(lanes == h, parts[h], total)
    return total


def commit_kernel(steps, heads, acum_ref, k_ref, v_ref, a_ref, b_ref, s_ref, out_ref, kbuf, pbuf, ubuf):
    seqs, cols, width = s_ref.shape
    group = cols // heads
    rows = steps * heads
    kbuf[...] = k_ref[...].astype(F32)
    for s in range(seqs):
        put(
            pbuf,
            pl.ds(s * rows, rows),
            dot_nt(k_ref[pl.ds(s * rows, rows), :], s_ref[s].astype(BF16)),
        )
    keys = [
        [kbuf[pl.ds(t * heads + h, seqs, stride=rows), :] for h in range(heads)] for t in range(steps)
    ]
    pairs = [(i, t) for t in range(steps) for i in range(t + 1)]
    products = [
        jnp.concatenate([keys[i][h] * keys[t][h] for h in range(heads)], axis=1) for i, t in pairs
    ]
    sums = jnp.dot(
        jnp.concatenate(products, axis=0).astype(BF16),
        block_ones(heads * width, width, cols, group),
        preferred_element_type=F32,
    )
    gram = {pair: sums[n * seqs : (n + 1) * seqs] for n, pair in enumerate(pairs)}
    norm = [lax.rsqrt(gram[(t, t)] + EPS) for t in range(steps)]
    decay = [a_ref[t] for t in range(steps)]
    fed = []
    through = None
    for t in range(steps):
        seen = own_head(
            [get(pbuf, pl.ds(t * heads + h, seqs, stride=rows), cols) for h in range(heads)], group
        )
        through = decay[t] if through is None else through * decay[t]
        fed = [decay[t] * f for f in fed]
        predicted = through * seen
        for i in range(t):
            predicted = predicted + gram[(i, t)] * fed[i]
        fed.append(b_ref[t] * (v_ref[t] - norm[t] * predicted) * norm[t])
    lanes = lane_group(seqs, cols, group)
    for t in range(steps):
        for h in range(heads):
            put(ubuf, pl.ds(t * heads + h, seqs, stride=rows), jnp.where(lanes == h, fed[t], 0.0))
    base = pl.program_id(0) * seqs
    for s in range(seqs):
        update = lax.dot_general(
            get(ubuf, pl.ds(s * rows, rows), cols).astype(BF16),
            k_ref[pl.ds(s * rows, rows), :],
            TN,
            preferred_element_type=F32,
        )
        for h in range(heads):
            span = slice(h * group, (h + 1) * group)
            out_ref[s, span, :] = acum_ref[(base + s) * heads + h] * s_ref[s, span, :] + update[span]


def commit(state, prev_keys, prev_values, retain, beta):
    seqs, steps, heads, width = prev_keys.shape
    group = state.shape[2]
    cols = heads * group
    block = 8
    rows = steps * heads

    def wide(x):
        x = jnp.transpose(x, (1, 0, 2))[..., None]
        return jnp.broadcast_to(x, (steps, seqs, heads, group)).reshape(steps, seqs, cols)

    values = jnp.transpose(prev_values, (1, 0, 2, 3)).astype(F32).reshape(steps, seqs, cols)
    acum = jnp.prod(retain, axis=1).reshape(-1)
    coef = pl.BlockSpec((steps, block, cols), lambda i: (0, i, 0))
    big = pl.BlockSpec((block, cols, width), lambda i: (i, 0, 0))
    return pl.pallas_call(
        functools.partial(commit_kernel, steps, heads),
        grid=(seqs // block,),
        out_shape=jax.ShapeDtypeStruct((seqs, cols, width), F32),
        in_specs=[
            pl.BlockSpec(memory_space=pltpu.SMEM),
            pl.BlockSpec((block * rows, width), lambda i: (i, 0)),
            coef,
            coef,
            coef,
            big,
        ],
        out_specs=big,
        scratch_shapes=[
            pltpu.VMEM((block * rows, width), F32),
            pltpu.VMEM((pl.cdiv(cols, 128), block * rows, 128), F32),
            pltpu.VMEM((pl.cdiv(cols, 128), block * rows, 128), F32),
        ],
    )(
        acum,
        prev_keys.reshape(seqs * rows, width),
        values,
        wide(retain),
        wide(beta),
        state.reshape(seqs, cols, width),
    )


def verify_kernel(
    nkv, heads, steps,
    tok_ref, gain_ref, wq_ref, wk_ref, wv_ref, wg_ref, wd_ref, wb_ref, rate_ref, hg_ref, wo_ref, st_ref,
    out_ref,
    xs, w, wo, st, acc, halves, kbuf, pbuf, ssend, srecv, psend, precv, part, zsend, zrecv,
    w_sem, big_sem, ag_send, ag_recv, fw_send, ex_send, ex_recv, p_send, p_recv, z_send, z_recv,
):
    kv, tp = lax.axis_index("kv"), lax.axis_index("tp")
    rows, feat = tok_ref.shape
    seqs, cols, width = st.shape
    group = cols // heads
    allheads = wd_ref.shape[0]
    partner = {"tp": 1 - tp}

    def far(d):
        return lax.rem(kv + d, nkv)

    hops = sorted(range(1, nkv), key=lambda d: (min(d, nkv - d), d))
    order = [(0, 0), (0, 1)] + [(d, e) for d in hops for e in (0, 1)]

    def owner(d, e):
        return far(d) * 2 + (tp if e == 0 else 1 - tp)

    def span(block):
        return pl.ds(pl.multiple_of(block * feat, 128), feat)

    mats = (wq_ref, wk_ref, wv_ref, wg_ref, wd_ref, wb_ref)
    tops = [0, cols, 2 * cols, 3 * cols, 4 * cols, 4 * cols + allheads]
    loads = []
    for n, (d, e) in enumerate(order):
        there = span(owner(d, e))
        chunk = []
        for m, ref in enumerate(mats):
            chunk.append(
                pltpu.make_async_copy(
                    ref.at[:, there], w.at[pl.ds(tops[m], ref.shape[0]), there], w_sem.at[n, m]
                )
            )
        loads.append(chunk)

    barrier = pltpu.get_barrier_semaphore()
    pl.semaphore_signal(barrier, inc=1, device_id=partner, device_id_type=MESH)
    for d in hops:
        pl.semaphore_signal(barrier, inc=1, device_id={"kv": far(d)}, device_id_type=MESH)
    for chunk in loads:
        for copy in chunk:
            copy.start()
    st_copy = pltpu.make_async_copy(st_ref, st, big_sem.at[0])
    wo_copy = pltpu.make_async_copy(wo_ref, wo, big_sem.at[1])
    st_copy.start()
    wo_copy.start()
    pl.semaphore_wait(barrier, nkv)

    def remote(src, dst, send, recv, where):
        return pltpu.make_async_remote_copy(
            src_ref=src, dst_ref=dst, send_sem=send, recv_sem=recv, device_id=where, device_id_type=MESH
        )

    mine = owner(0, 0)
    pending = []
    for d in hops:
        copy = remote(tok_ref, xs.at[mine], ag_send.at[d], ag_recv.at[mine], {"kv": far(d)})
        copy.start()
        pending.append(copy)
    copy = remote(tok_ref, xs.at[mine], ag_send.at[0], ag_recv.at[mine], partner)
    copy.start()
    pending.append(copy)

    square = jnp.zeros((rows, 1), F32)
    for n, (d, e) in enumerate(order):
        block = owner(d, e)
        if n == 0:
            x = tok_ref[...]
        else:
            remote(tok_ref, xs.at[block], ag_send.at[0], ag_recv.at[block], partner).wait_recv()
            if e == 0:
                copy = remote(xs.at[block], xs.at[block], fw_send.at[d], ag_recv.at[block], partner)
                copy.start()
                pending.append(copy)
            x = xs[block]
        x = x.astype(F32)
        square = square + jnp.sum(x * x, axis=1, keepdims=True)
        xg = (x * gain_ref[:, span(block)]).astype(BF16)
        for copy in loads[n]:
            copy.wait()
        product = dot_nt(xg, w[:, span(block)])
        if n == 0:
            acc[...] = product
        else:
            acc[...] += product
    scale = lax.rsqrt(square / (feat * nkv * 2) + EPS)

    halves[tp] = (acc[:, : 2 * cols] * scale).astype(BF16)
    qk = remote(halves.at[tp], halves.at[tp], ex_send.at[0], ex_recv.at[0], partner)
    qk.start()
    pending_tail = [qk]

    value = silu((acc[:, 2 * cols : 3 * cols] * scale).astype(BF16).astype(F32))
    gate = silu((acc[:, 3 * cols : 4 * cols] * scale).astype(BF16).astype(F32)) * hg_ref[...]
    pre = acc[:, 4 * cols :] * scale
    pick_row = lax.broadcasted_iota(jnp.int32, (allheads, cols), 0)
    pick = (pick_row == kv * heads + lane_group(allheads, cols, group)).astype(F32)
    dec = jnp.dot(pre[:, :allheads], pick, precision=lax.Precision.HIGHEST, preferred_element_type=F32)
    bet = jnp.dot(pre[:, allheads:], pick, precision=lax.Precision.HIGHEST, preferred_element_type=F32)
    soft = jnp.maximum(dec, 0.0) + jnp.log1p(jnp.exp(-jnp.abs(dec)))
    retain = jnp.exp(-(rate_ref[...] * soft))
    strength = jax.nn.sigmoid(bet)
    ones_wide = block_ones(heads * width, width, cols, group)
    ones_cols = block_ones(cols, group, cols, group)

    def at(x, t):
        return x[t * seqs : (t + 1) * seqs]

    remote(halves.at[1 - tp], halves.at[1 - tp], ex_send.at[0], ex_recv.at[0], partner).wait_recv()
    low, high = halves[0].astype(F32), halves[1].astype(F32)
    low, high = silu(low), silu(high)

    def whole(kind):
        base = kind * cols
        pieces = []
        for h in range(heads):
            lanes = slice(base + h * group, base + (h + 1) * group)
            pieces += [low[:, lanes], high[:, lanes]]
        return jnp.concatenate(pieces, axis=1)

    query, key = whole(0), whole(1)
    for t in range(steps):
        for h in range(heads):
            lanes = slice(h * width, (h + 1) * width)
            place = (h * 2) * steps + t
            kbuf[pl.ds(place, seqs, stride=heads * 2 * steps), :] = at(key, t)[:, lanes]
            kbuf[pl.ds(place + steps, seqs, stride=heads * 2 * steps), :] = at(query, t)[:, lanes]
    st_copy.wait()
    tall = 2 * steps
    for s in range(seqs):
        stacked = kbuf[pl.ds(s * heads * tall, heads * tall), :].astype(BF16)
        seen = dot_nt(stacked, st[s].astype(BF16))
        put(
            pbuf,
            pl.ds(s * tall, tall),
            own_head([seen[h * tall : (h + 1) * tall] for h in range(heads)], group),
        )
    pairs = [("k", i, t) for t in range(steps) for i in range(t + 1)]
    pairs += [("q", i, t) for t in range(steps) for i in range(t + 1)]
    products = [at(key, i) * at(key if kind == "k" else query, t) for kind, i, t in pairs]
    products.append(query * query)
    sums = jnp.dot(
        jnp.concatenate(products, axis=0).astype(BF16), ones_wide, preferred_element_type=F32
    )
    gram = {pair: at(sums, n) for n, pair in enumerate(pairs)}
    qsq = sums[len(pairs) * seqs :]
    qnorm = lax.rsqrt(qsq + EPS) * width ** (-0.5)
    fed, through, outs = [], None, []
    for t in range(steps):
        norm = lax.rsqrt(gram[("k", t, t)] + EPS)
        a = at(retain, t)
        through = a if through is None else through * a
        fed = [a * f for f in fed]
        predicted = through * get(pbuf, pl.ds(t, seqs, stride=tall), cols)
        for i in range(t):
            predicted = predicted + gram[("k", i, t)] * fed[i]
        fed.append(at(strength, t) * (at(value, t) - norm * predicted) * norm)
        o = through * get(pbuf, pl.ds(steps + t, seqs, stride=tall), cols)
        for i in range(t + 1):
            o = o + gram[("q", i, t)] * fed[i]
        outs.append(o * at(qnorm, t))
    heads_out = jnp.concatenate(outs, axis=0)
    squares = jnp.dot((heads_out * heads_out).astype(BF16), ones_cols, preferred_element_type=F32)
    ssend[...] = squares
    sq = remote(ssend, srecv, ex_send.at[1], ex_recv.at[1], partner)
    sq.start()
    ready = heads_out * gate
    wo_copy.wait()
    sq.wait_recv()
    pending_tail.append(sq)
    total = squares + srecv[...]
    scaled = (ready * lax.rsqrt(total / (2 * group) + EPS)).astype(BF16)

    targets = sorted(range(1, nkv), key=lambda d: (-min(d, nkv - d), d)) + [0]
    crossing = []
    for j, d in enumerate(targets):
        psend[j] = jnp.dot(scaled, wo[:, span(owner(d, 1))], preferred_element_type=F32).astype(BF16)
        copy = remote(psend.at[j], precv.at[j], p_send.at[j], p_recv.at[j], partner)
        copy.start()
        crossing.append(copy)
        part[j] = jnp.dot(scaled, wo[:, span(owner(d, 0))], preferred_element_type=F32)
    flights = []
    for j, d in enumerate(targets):
        crossing[j].wait_recv()
        both = part[j] + precv[j].astype(F32)
        if d:
            zsend[j] = both.astype(BF16)
            copy = remote(zsend.at[j], zrecv.at[j], z_send.at[j], z_recv.at[j], {"kv": far(d)})
            copy.start()
            flights.append(copy)
    mixed = both
    for j, copy in sorted(enumerate(flights), key=lambda f: -f[0]):
        copy.wait_recv()
        mixed = mixed + zrecv[j].astype(F32)
    out_ref[...] = mixed.astype(BF16)
    for copy in pending + pending_tail + crossing + flights:
        copy.wait_send()


def local(
    nkv,
    tokens,
    norm_gain,
    w_query,
    w_key,
    w_value,
    w_gate,
    w_decay,
    w_beta,
    decay_rate,
    head_gain,
    w_out,
    state,
    prev_keys,
    prev_values,
    prev_decay,
    prev_beta,
    accepted,
):
    seqs, steps, feat = tokens.shape
    heads, group, width = state.shape[1:]
    cols = heads * group
    rows = seqs * steps
    full = norm_gain.shape[0]
    allheads = w_decay.shape[1]
    mask = (jnp.arange(steps)[None, :] < accepted[:, None]).astype(F32)[:, :, None]
    committed = commit(state, prev_keys, prev_values, jnp.exp(-prev_decay * mask), prev_beta * mask)

    vmem = pl.BlockSpec(memory_space=pltpu.VMEM)
    hbm = pl.BlockSpec(memory_space=pl.ANY)
    blocks = 2 * nkv
    tall = 2 * steps
    DMA = pltpu.SemaphoreType.DMA
    mixed = pl.pallas_call(
        functools.partial(verify_kernel, nkv, heads, steps),
        out_shape=jax.ShapeDtypeStruct((rows, feat), BF16),
        in_specs=[vmem, vmem] + [hbm] * 6 + [vmem, vmem] + [hbm] * 2,
        out_specs=vmem,
        scratch_shapes=[
            pltpu.VMEM((blocks, rows, feat), BF16),
            pltpu.VMEM((4 * cols + 2 * allheads, full), BF16),
            pltpu.VMEM((cols, full), BF16),
            pltpu.VMEM((seqs, cols, width), F32),
            pltpu.VMEM((rows, 4 * cols + 2 * allheads), F32),
            pltpu.VMEM((2, rows, 2 * cols), BF16),
            pltpu.VMEM((seqs * heads * tall, width), F32),
            pltpu.VMEM((pl.cdiv(cols, 128), seqs * tall, 128), F32),
            pltpu.VMEM((rows, cols), F32),
            pltpu.VMEM((rows, cols), F32),
            pltpu.VMEM((nkv, rows, feat), BF16),
            pltpu.VMEM((nkv, rows, feat), BF16),
            pltpu.VMEM((nkv, rows, feat), F32),
            pltpu.VMEM((nkv, rows, feat), BF16),
            pltpu.VMEM((nkv, rows, feat), BF16),
            DMA((blocks, 6)),
            DMA((2,)),
            DMA((nkv,)),
            DMA((blocks,)),
            DMA((nkv,)),
            DMA((2,)),
            DMA((2,)),
            DMA((nkv,)),
            DMA((nkv,)),
            DMA((nkv,)),
            DMA((nkv,)),
        ],
        compiler_params=pltpu.CompilerParams(
            collective_id=0, has_side_effects=True, vmem_limit_bytes=60 * 1024 * 1024
        ),
    )(
        jnp.transpose(tokens, (1, 0, 2)).reshape(rows, feat),
        norm_gain.reshape(1, full),
        w_query.reshape(cols, full),
        w_key.reshape(cols, full),
        w_value.reshape(cols, full),
        w_gate.reshape(cols, full),
        w_decay.T,
        w_beta.T,
        jnp.repeat(decay_rate, group).reshape(1, cols),
        jnp.tile(head_gain, heads).reshape(1, cols),
        w_out.reshape(cols, full),
        committed,
    )
    mixed = jnp.transpose(mixed.reshape(steps, seqs, feat), (1, 0, 2))
    return mixed, committed.reshape(state.shape)


def solution(mesh):
    in_specs = (
        P(("grp", "dp"), None, ("kv", "tp")),
        P(),
        P("kv", "tp", None),
        P("kv", "tp", None),
        P("kv", "tp", None),
        P("kv", "tp", None),
        P(),
        P(),
        P("kv"),
        P("tp"),
        P("kv", "tp", None),
        P(("grp", "dp"), "kv", "tp", None),
        P(("grp", "dp"), None, "kv", None),
        P(("grp", "dp"), None, "kv", "tp"),
        P(("grp", "dp"), None, "kv"),
        P(("grp", "dp"), None, "kv"),
        P(("grp", "dp")),
    )
    out_specs = (P(("grp", "dp"), None, ("kv", "tp")), P(("grp", "dp"), "kv", "tp", None))
    return jax.shard_map(
        functools.partial(local, mesh.shape["kv"]),
        mesh=mesh, in_specs=in_specs, out_specs=out_specs, check_vma=False,
    )
```

```python
import functools

import jax
import jax.numpy as jnp
from jax import lax
from jax.experimental import pallas as pl
from jax.experimental.pallas import tpu as pltpu
from jax.sharding import PartitionSpec as P

EPS = 1e-06
F32 = jnp.float32
BF16 = jnp.bfloat16
MESH = pl.DeviceIdType.MESH
NT = (((1,), (1,)), ((), ()))
TN = (((0,), (0,)), ((), ()))


def dot_nt(a, b):
    return lax.dot_general(a, b, NT, preferred_element_type=F32)


def silu(u):
    return u * jax.nn.sigmoid(u)


def lane_group(rows, cols, group):
    return lax.broadcasted_iota(jnp.int32, (rows, cols), 1) // group


def block_ones(rows, row_group, cols, col_group):
    r = lax.broadcasted_iota(jnp.int32, (rows, cols), 0) // row_group
    return (r == lane_group(rows, cols, col_group)).astype(F32).astype(BF16)


def put(buf, rows, x):
    cols = x.shape[1]
    if cols < 128:
        x = jnp.concatenate([x] * (128 // cols), axis=1)
    for c in range(buf.shape[0]):
        buf[c, rows, :] = x[:, c * 128 : (c + 1) * 128]


def get(buf, rows, cols):
    x = jnp.concatenate([buf[c, rows, :] for c in range(buf.shape[0])], axis=1)
    return x[:, :cols]


def own_head(parts, group):
    rows, cols = parts[0].shape
    if len(parts) == 1:
        return parts[0]
    lanes = lane_group(rows, cols, group)
    total = jnp.where(lanes == 0, parts[0], 0.0)
    for h in range(1, len(parts)):
        total = jnp.where(lanes == h, parts[h], total)
    return total


def commit_kernel(steps, heads, k_ref, v_ref, pd_ref, pb_ref, acc_ref, s_ref, out_ref, kbuf, vbuf, pbuf, ubuf, coef):
    seqs, cols, width = s_ref.shape
    group = cols // heads
    rows = steps * heads
    total = acc_ref.shape[1]

    @pl.when(pl.program_id(0) == 0)
    def _():
        step_of = lax.broadcasted_iota(jnp.int32, (rows, total), 0) // heads
        mask = (step_of < acc_ref[...]).astype(F32)
        retain = jnp.exp(-pd_ref[...] * mask)
        beta = pb_ref[...] * mask
        head_of = lax.broadcasted_iota(jnp.int32, (rows, cols), 0)
        for t in range(steps):
            pick = (head_of == t * heads + lane_group(rows, cols, group)).astype(F32)
            for n, x in enumerate((retain, beta)):
                coef[n * steps + t] = lax.dot_general(
                    x, pick, TN, precision=lax.Precision.HIGHEST, preferred_element_type=F32
                )

    kbuf[...] = k_ref[...].astype(F32)
    values = v_ref[...].astype(F32)
    vbuf[...] = jnp.concatenate([values] * (width // group), axis=1)
    for s in range(seqs):
        put(
            pbuf,
            pl.ds(s * rows, rows),
            dot_nt(k_ref[pl.ds(s * rows, rows), :], s_ref[s].astype(BF16)),
        )

    def every(t, h):
        return pl.ds(t * heads + h, seqs, stride=rows)

    keys = [[kbuf[every(t, h), :] for h in range(heads)] for t in range(steps)]
    pairs = [(i, t) for t in range(steps) for i in range(t + 1)]
    products = [
        jnp.concatenate([keys[i][h] * keys[t][h] for h in range(heads)], axis=1) for i, t in pairs
    ]
    sums = jnp.dot(
        jnp.concatenate(products, axis=0).astype(BF16),
        block_ones(heads * width, width, cols, group),
        preferred_element_type=F32,
    )
    gram = {pair: sums[n * seqs : (n + 1) * seqs] for n, pair in enumerate(pairs)}
    norm = [lax.rsqrt(gram[(t, t)] + EPS) for t in range(steps)]
    here = pl.ds(pl.multiple_of(pl.program_id(0) * seqs, seqs), seqs)
    fed = []
    through = None
    copies = max(1, cols // width)
    for t in range(steps):
        decay = coef[t, here, :]
        seen = own_head([get(pbuf, every(t, h), cols) for h in range(heads)], group)
        value = own_head(
            [jnp.concatenate([vbuf[every(t, h), :]] * copies, axis=1)[:, :cols] for h in range(heads)],
            group,
        )
        through = decay if through is None else through * decay
        fed = [decay * f for f in fed]
        predicted = through * seen
        for i in range(t):
            predicted = predicted + gram[(i, t)] * fed[i]
        fed.append(coef[steps + t, here, :] * (value - norm[t] * predicted) * norm[t])
    lanes = lane_group(seqs, cols, group)
    for t in range(steps):
        for h in range(heads):
            put(ubuf, every(t, h), jnp.where(lanes == h, fed[t], 0.0))
    for s in range(seqs):
        update = lax.dot_general(
            get(ubuf, pl.ds(s * rows, rows), cols).astype(BF16),
            k_ref[pl.ds(s * rows, rows), :],
            TN,
            preferred_element_type=F32,
        )
        for h in range(heads):
            span = slice(h * group, (h + 1) * group)
            kept = through[s : s + 1, h * group : h * group + 1]
            out_ref[s, span, :] = kept * s_ref[s, span, :] + update[span]


def commit(state, prev_keys, prev_values, prev_decay, prev_beta, accepted):
    seqs, steps, heads, width = prev_keys.shape
    group = state.shape[2]
    cols = heads * group
    block = 8
    rows = steps * heads
    big = pl.BlockSpec((block, cols, width), lambda i: (i, 0, 0))
    coef = pl.BlockSpec((rows, seqs), lambda i: (0, 0))
    tiles = pl.cdiv(cols, 128)
    return pl.pallas_call(
        functools.partial(commit_kernel, steps, heads),
        grid=(seqs // block,),
        out_shape=jax.ShapeDtypeStruct((seqs, cols, width), F32),
        in_specs=[
            pl.BlockSpec((block * rows, width), lambda i: (i, 0)),
            pl.BlockSpec((block * rows, group), lambda i: (i, 0)),
            coef,
            coef,
            pl.BlockSpec((1, seqs), lambda i: (0, 0)),
            big,
        ],
        out_specs=big,
        scratch_shapes=[
            pltpu.VMEM((block * rows, width), F32),
            pltpu.VMEM((block * rows, width), F32),
            pltpu.VMEM((tiles, block * rows, 128), F32),
            pltpu.VMEM((tiles, block * rows, 128), F32),
            pltpu.VMEM((2 * steps, seqs, cols), F32),
        ],
        cost_estimate=pl.CostEstimate(
            flops=4 * seqs * rows * cols * width, bytes_accessed=8 * state.size, transcendentals=0
        ),
    )(
        prev_keys.reshape(seqs * rows, width),
        prev_values.reshape(seqs * rows, group),
        jnp.transpose(prev_decay, (1, 2, 0)).reshape(rows, seqs),
        jnp.transpose(prev_beta, (1, 2, 0)).reshape(rows, seqs),
        accepted.reshape(1, seqs),
        state.reshape(seqs, cols, width),
    )


def verify_kernel(
    nkv, heads, steps, tok_ref, *refs
):
    got, refs = refs[: nkv - 1], refs[nkv - 1 :]
    verify(nkv, heads, steps, (tok_ref, *got), *refs)


def verify(
    nkv, heads, steps,
    got, gain_ref, wq_ref, wk_ref, wv_ref, wg_ref, wd_ref, wb_ref, rate_ref, hg_ref, wo_ref, st_ref,
    out_ref,
    xs, w, wo, st, acc, halves, kbuf, pbuf, ssend, srecv, psend, precv, part, zsend, zrecv,
    w_sem, big_sem, ag_send, ag_recv, ex_send, ex_recv, p_send, p_recv, z_send, z_recv,
):
    kv, tp = lax.axis_index("kv"), lax.axis_index("tp")
    rows, feat = got[0].shape
    seqs, cols, width = st.shape
    group = cols // heads
    allheads = wd_ref.shape[0]
    partner = {"tp": 1 - tp}

    def far(d):
        return lax.rem(kv + d, nkv)

    hops = sorted(range(1, nkv), key=lambda d: (min(d, nkv - d), d))
    order = [(d, e) for e in (0, 1) for d in [0] + hops]

    def owner(d, e):
        return far(d) * 2 + (tp if e == 0 else 1 - tp)

    def span(block):
        return pl.ds(pl.multiple_of(block * feat, 128), feat)

    mats = (wq_ref, wk_ref, wv_ref, wg_ref, wd_ref, wb_ref)
    tops = [0, cols, 2 * cols, 3 * cols, 4 * cols, 4 * cols + allheads]
    loads = []
    for n, (d, e) in enumerate(order):
        there = span(owner(d, e))
        chunk = []
        for m, ref in enumerate(mats):
            chunk.append(
                pltpu.make_async_copy(
                    ref.at[:, there], w.at[pl.ds(tops[m], ref.shape[0]), there], w_sem.at[n, m]
                )
            )
        loads.append(chunk)

    barrier = pltpu.get_barrier_semaphore()
    pl.semaphore_signal(barrier, inc=1, device_id=partner, device_id_type=MESH)
    for d in hops:
        pl.semaphore_signal(barrier, inc=1, device_id={"kv": far(d)}, device_id_type=MESH)
    for chunk in loads:
        for copy in chunk:
            copy.start()
    st_copy = pltpu.make_async_copy(st_ref, st, big_sem.at[0])
    wo_copy = pltpu.make_async_copy(wo_ref, wo, big_sem.at[1])
    st_copy.start()
    wo_copy.start()
    pl.semaphore_wait(barrier, nkv)

    def remote(src, dst, send, recv, where):
        return pltpu.make_async_remote_copy(
            src_ref=src, dst_ref=dst, send_sem=send, recv_sem=recv, device_id=where, device_id_type=MESH
        )

    pending = []
    for d in [0] + hops:
        copy = remote(got[d], xs.at[d], ag_send.at[d], ag_recv.at[d], partner)
        copy.start()
        pending.append(copy)

    square = jnp.zeros((rows, 1), F32)
    for n, (d, e) in enumerate(order):
        block = owner(d, e)
        if e == 0:
            x = got[d][...]
        else:
            pending[[0, *hops].index(d)].wait_recv()
            x = xs[d]
        x = x.astype(F32)
        square = square + jnp.sum(x * x, axis=1, keepdims=True)
        xg = (x * gain_ref[:, span(block)]).astype(BF16)
        for copy in loads[n]:
            copy.wait()
        product = dot_nt(xg, w[:, span(block)])
        if n == 0:
            acc[...] = product
        else:
            acc[...] += product
    scale = lax.rsqrt(square / (feat * nkv * 2) + EPS)

    halves[tp] = (acc[:, : 2 * cols] * scale).astype(BF16)
    qk = remote(halves.at[tp], halves.at[tp], ex_send.at[0], ex_recv.at[0], partner)
    qk.start()
    pending_tail = [qk]

    value = silu((acc[:, 2 * cols : 3 * cols] * scale).astype(BF16).astype(F32))
    gate = silu((acc[:, 3 * cols : 4 * cols] * scale).astype(BF16).astype(F32)) * jnp.concatenate([hg_ref[...]] * heads, axis=1)
    pre = acc[:, 4 * cols :] * scale
    pick_row = lax.broadcasted_iota(jnp.int32, (allheads, cols), 0)
    pick = (pick_row == kv * heads + lane_group(allheads, cols, group)).astype(F32)
    dec = jnp.dot(pre[:, :allheads], pick, precision=lax.Precision.HIGHEST, preferred_element_type=F32)
    bet = jnp.dot(pre[:, allheads:], pick, precision=lax.Precision.HIGHEST, preferred_element_type=F32)
    lanes_own = lane_group(1, cols, group)
    rate = jnp.zeros((1, cols), F32)
    for h in range(heads):
        rate = jnp.where(lanes_own == h, rate_ref[:, h : h + 1], rate)
    soft = jnp.maximum(dec, 0.0) + jnp.log1p(jnp.exp(-jnp.abs(dec)))
    retain = jnp.exp(-(rate * soft))
    strength = jax.nn.sigmoid(bet)
    ones_wide = block_ones(heads * width, width, cols, group)
    ones_cols = block_ones(cols, group, cols, group)

    def at(x, t):
        return x[t * seqs : (t + 1) * seqs]

    remote(halves.at[1 - tp], halves.at[1 - tp], ex_send.at[0], ex_recv.at[0], partner).wait_recv()
    low, high = halves[0].astype(F32), halves[1].astype(F32)
    low, high = silu(low), silu(high)

    def whole(kind):
        base = kind * cols
        pieces = []
        for h in range(heads):
            lanes = slice(base + h * group, base + (h + 1) * group)
            pieces += [low[:, lanes], high[:, lanes]]
        return jnp.concatenate(pieces, axis=1)

    query, key = whole(0), whole(1)
    for t in range(steps):
        for h in range(heads):
            lanes = slice(h * width, (h + 1) * width)
            place = (h * 2) * steps + t
            kbuf[pl.ds(place, seqs, stride=heads * 2 * steps), :] = at(key, t)[:, lanes]
            kbuf[pl.ds(place + steps, seqs, stride=heads * 2 * steps), :] = at(query, t)[:, lanes]
    st_copy.wait()
    tall = 2 * steps
    for s in range(seqs):
        stacked = kbuf[pl.ds(s * heads * tall, heads * tall), :].astype(BF16)
        seen = dot_nt(stacked, st[s].astype(BF16))
        put(
            pbuf,
            pl.ds(s * tall, tall),
            own_head([seen[h * tall : (h + 1) * tall] for h in range(heads)], group),
        )
    pairs = [("k", i, t) for t in range(steps) for i in range(t + 1)]
    pairs += [("q", i, t) for t in range(steps) for i in range(t + 1)]
    products = [at(key, i) * at(key if kind == "k" else query, t) for kind, i, t in pairs]
    products.append(query * query)
    sums = jnp.dot(
        jnp.concatenate(products, axis=0).astype(BF16), ones_wide, preferred_element_type=F32
    )
    gram = {pair: at(sums, n) for n, pair in enumerate(pairs)}
    qsq = sums[len(pairs) * seqs :]
    qnorm = lax.rsqrt(qsq + EPS) * width ** (-0.5)
    fed, through, outs = [], None, []
    for t in range(steps):
        norm = lax.rsqrt(gram[("k", t, t)] + EPS)
        a = at(retain, t)
        through = a if through is None else through * a
        fed = [a * f for f in fed]
        predicted = through * get(pbuf, pl.ds(t, seqs, stride=tall), cols)
        for i in range(t):
            predicted = predicted + gram[("k", i, t)] * fed[i]
        fed.append(at(strength, t) * (at(value, t) - norm * predicted) * norm)
        o = through * get(pbuf, pl.ds(steps + t, seqs, stride=tall), cols)
        for i in range(t + 1):
            o = o + gram[("q", i, t)] * fed[i]
        outs.append(o * at(qnorm, t))
    heads_out = jnp.concatenate(outs, axis=0)
    squares = jnp.dot((heads_out * heads_out).astype(BF16), ones_cols, preferred_element_type=F32)
    ssend[...] = squares
    sq = remote(ssend, srecv, ex_send.at[1], ex_recv.at[1], partner)
    sq.start()
    ready = heads_out * gate
    wo_copy.wait()
    sq.wait_recv()
    pending_tail.append(sq)
    total = squares + srecv[...]
    scaled = (ready * lax.rsqrt(total / (2 * group) + EPS)).astype(BF16)

    targets = sorted(range(1, nkv), key=lambda d: (-min(d, nkv - d), d)) + [0]
    crossing = []
    for j, d in enumerate(targets):
        psend[j] = jnp.dot(scaled, wo[:, span(owner(d, 1))], preferred_element_type=F32).astype(BF16)
        copy = remote(psend.at[j], precv.at[j], p_send.at[j], p_recv.at[j], partner)
        copy.start()
        crossing.append(copy)
        part[j] = jnp.dot(scaled, wo[:, span(owner(d, 0))], preferred_element_type=F32)
    flights = []
    for j, d in enumerate(targets):
        crossing[j].wait_recv()
        both = part[j] + precv[j].astype(F32)
        if d:
            zsend[j] = both.astype(BF16)
            copy = remote(zsend.at[j], zrecv.at[j], z_send.at[j], z_recv.at[j], {"kv": far(d)})
            copy.start()
            flights.append(copy)
    mixed = both
    for j, copy in sorted(enumerate(flights), key=lambda f: -f[0]):
        copy.wait_recv()
        mixed = mixed + zrecv[j].astype(F32)
    out_ref[...] = mixed.astype(BF16)
    for copy in pending + pending_tail + crossing + flights:
        copy.wait_send()


def local(
    nkv,
    tokens,
    norm_gain,
    w_query,
    w_key,
    w_value,
    w_gate,
    w_decay,
    w_beta,
    decay_rate,
    head_gain,
    w_out,
    state,
    prev_keys,
    prev_values,
    prev_decay,
    prev_beta,
    accepted,
):
    seqs, steps, feat = tokens.shape
    heads, group, width = state.shape[1:]
    cols = heads * group
    rows = seqs * steps
    full = norm_gain.shape[0]
    allheads = w_decay.shape[1]
    flat = jnp.transpose(tokens, (1, 0, 2)).reshape(rows, feat)
    got = [
        lax.ppermute(flat, "kv", [((i + d) % nkv, i) for i in range(nkv)]) for d in range(1, nkv)
    ]
    committed = commit(state, prev_keys, prev_values, prev_decay, prev_beta, accepted)

    vmem = pl.BlockSpec(memory_space=pltpu.VMEM)
    hbm = pl.BlockSpec(memory_space=pl.ANY)
    blocks = 2 * nkv
    tall = 2 * steps
    DMA = pltpu.SemaphoreType.DMA
    mixed = pl.pallas_call(
        functools.partial(verify_kernel, nkv, heads, steps),
        out_shape=jax.ShapeDtypeStruct((rows, feat), BF16),
        in_specs=[vmem] * (nkv + 1) + [hbm] * 6 + [vmem, vmem] + [hbm] * 2,
        out_specs=vmem,
        scratch_shapes=[
            pltpu.VMEM((nkv, rows, feat), BF16),
            pltpu.VMEM((4 * cols + 2 * allheads, full), BF16),
            pltpu.VMEM((cols, full), BF16),
            pltpu.VMEM((seqs, cols, width), F32),
            pltpu.VMEM((rows, 4 * cols + 2 * allheads), F32),
            pltpu.VMEM((2, rows, 2 * cols), BF16),
            pltpu.VMEM((seqs * heads * tall, width), F32),
            pltpu.VMEM((pl.cdiv(cols, 128), seqs * tall, 128), F32),
            pltpu.VMEM((rows, cols), F32),
            pltpu.VMEM((rows, cols), F32),
            pltpu.VMEM((nkv, rows, feat), BF16),
            pltpu.VMEM((nkv, rows, feat), BF16),
            pltpu.VMEM((nkv, rows, feat), F32),
            pltpu.VMEM((nkv, rows, feat), BF16),
            pltpu.VMEM((nkv, rows, feat), BF16),
            DMA((blocks, 6)),
            DMA((2,)),
            DMA((nkv,)),
            DMA((nkv,)),
            DMA((2,)),
            DMA((2,)),
            DMA((nkv,)),
            DMA((nkv,)),
            DMA((nkv,)),
            DMA((nkv,)),
        ],
        compiler_params=pltpu.CompilerParams(
            collective_id=0, has_side_effects=True, vmem_limit_bytes=40 * 1024 * 1024
        ),
    )(
        flat,
        *got,
        norm_gain.reshape(1, full),
        w_query.reshape(cols, full),
        w_key.reshape(cols, full),
        w_value.reshape(cols, full),
        w_gate.reshape(cols, full),
        w_decay.T,
        w_beta.T,
        decay_rate.reshape(1, heads),
        head_gain.reshape(1, group),
        w_out.reshape(cols, full),
        committed,
    )
    mixed = jnp.transpose(mixed.reshape(steps, seqs, feat), (1, 0, 2))
    return mixed, committed.reshape(state.shape)


def solution(mesh):
    in_specs = (
        P(("grp", "dp"), None, ("kv", "tp")),
        P(),
        P("kv", "tp", None),
        P("kv", "tp", None),
        P("kv", "tp", None),
        P("kv", "tp", None),
        P(),
        P(),
        P("kv"),
        P("tp"),
        P("kv", "tp", None),
        P(("grp", "dp"), "kv", "tp", None),
        P(("grp", "dp"), None, "kv", None),
        P(("grp", "dp"), None, "kv", "tp"),
        P(("grp", "dp"), None, "kv"),
        P(("grp", "dp"), None, "kv"),
        P(("grp", "dp")),
    )
    out_specs = (P(("grp", "dp"), None, ("kv", "tp")), P(("grp", "dp"), "kv", "tp", None))
    return jax.shard_map(
        functools.partial(local, mesh.shape["kv"]),
        mesh=mesh, in_specs=in_specs, out_specs=out_specs, check_vma=False,
    )
```

```python
import functools

import jax
import jax.numpy as jnp
from jax import lax
from jax.experimental import pallas as pl
from jax.experimental.pallas import tpu as pltpu
from jax.sharding import PartitionSpec as P

EPS = 1e-06
F32 = jnp.float32
BF16 = jnp.bfloat16
MESH = pl.DeviceIdType.MESH
NT = (((1,), (1,)), ((), ()))
TN = (((0,), (0,)), ((), ()))


def dot_nt(a, b):
    return lax.dot_general(a, b, NT, preferred_element_type=F32)


def silu(u):
    return u * jax.nn.sigmoid(u)


def lane_group(rows, cols, group):
    return lax.broadcasted_iota(jnp.int32, (rows, cols), 1) // group


def block_ones(rows, row_group, cols, col_group):
    r = lax.broadcasted_iota(jnp.int32, (rows, cols), 0) // row_group
    return (r == lane_group(rows, cols, col_group)).astype(F32).astype(BF16)


def put(buf, rows, x):
    cols = x.shape[1]
    if cols < 128:
        x = jnp.concatenate([x] * (128 // cols), axis=1)
    for c in range(buf.shape[0]):
        buf[c, rows, :] = x[:, c * 128 : (c + 1) * 128]


def get(buf, rows, cols):
    x = jnp.concatenate([buf[c, rows, :] for c in range(buf.shape[0])], axis=1)
    return x[:, :cols]


def own_head(parts, group):
    rows, cols = parts[0].shape
    if len(parts) == 1:
        return parts[0]
    lanes = lane_group(rows, cols, group)
    total = jnp.where(lanes == 0, parts[0], 0.0)
    for h in range(1, len(parts)):
        total = jnp.where(lanes == h, parts[h], total)
    return total


def coefficients(steps, heads, cols, pd_ref, pb_ref, acc_ref, coef):
    rows = steps * heads
    group = cols // heads
    total = acc_ref.shape[1]
    step_of = lax.broadcasted_iota(jnp.int32, (rows, total), 0) // heads
    mask = (step_of < acc_ref[...]).astype(F32)
    retain = jnp.exp(-pd_ref[...] * mask)
    beta = pb_ref[...] * mask
    head_of = lax.broadcasted_iota(jnp.int32, (rows, cols), 0)
    for t in range(steps):
        pick = (head_of == t * heads + lane_group(rows, cols, group)).astype(F32)
        for n, x in enumerate((retain, beta)):
            coef[n * steps + t] = lax.dot_general(
                x, pick, TN, precision=lax.Precision.HIGHEST, preferred_element_type=F32
            )


def commit_block(steps, heads, block, k_ref, v_ref, s_ref, out_ref, kbuf, vbuf, pbuf, ubuf, coef):
    seqs, cols, width = s_ref.shape
    group = cols // heads
    rows = steps * heads
    kbuf[...] = k_ref[...].astype(F32)
    values = v_ref[...].astype(F32)
    vbuf[...] = jnp.concatenate([values] * (width // group), axis=1)
    for s in range(seqs):
        put(
            pbuf,
            pl.ds(s * rows, rows),
            dot_nt(k_ref[pl.ds(s * rows, rows), :], s_ref[s].astype(BF16)),
        )

    def every(t, h):
        return pl.ds(t * heads + h, seqs, stride=rows)

    keys = [[kbuf[every(t, h), :] for h in range(heads)] for t in range(steps)]
    pairs = [(i, t) for t in range(steps) for i in range(t + 1)]
    products = [
        jnp.concatenate([keys[i][h] * keys[t][h] for h in range(heads)], axis=1) for i, t in pairs
    ]
    sums = jnp.dot(
        jnp.concatenate(products, axis=0).astype(BF16),
        block_ones(heads * width, width, cols, group),
        preferred_element_type=F32,
    )
    gram = {pair: sums[n * seqs : (n + 1) * seqs] for n, pair in enumerate(pairs)}
    norm = [lax.rsqrt(gram[(t, t)] + EPS) for t in range(steps)]
    here = pl.ds(block * seqs, seqs)
    fed = []
    through = None
    copies = max(1, cols // width)
    for t in range(steps):
        decay = coef[t, here, :]
        seen = own_head([get(pbuf, every(t, h), cols) for h in range(heads)], group)
        value = own_head(
            [jnp.concatenate([vbuf[every(t, h), :]] * copies, axis=1)[:, :cols] for h in range(heads)],
            group,
        )
        through = decay if through is None else through * decay
        fed = [decay * f for f in fed]
        predicted = through * seen
        for i in range(t):
            predicted = predicted + gram[(i, t)] * fed[i]
        fed.append(coef[steps + t, here, :] * (value - norm[t] * predicted) * norm[t])
    lanes = lane_group(seqs, cols, group)
    for t in range(steps):
        for h in range(heads):
            put(ubuf, every(t, h), jnp.where(lanes == h, fed[t], 0.0))
    for s in range(seqs):
        update = lax.dot_general(
            get(ubuf, pl.ds(s * rows, rows), cols).astype(BF16),
            k_ref[pl.ds(s * rows, rows), :],
            TN,
            preferred_element_type=F32,
        )
        for h in range(heads):
            span = slice(h * group, (h + 1) * group)
            kept = through[s : s + 1, h * group : h * group + 1]
            out_ref[s, span, :] = kept * s_ref[s, span, :] + update[span]


def verify_kernel(
    nkv, heads, steps,
    tok_ref, gain_ref, wq_ref, wk_ref, wv_ref, wg_ref, wd_ref, wb_ref, rate_ref, hg_ref, wo_ref, st_ref,
    ok_ref, ov_ref, pd_ref, pb_ref, acc_ref,
    out_ref, com_ref,
    xs, w, wo, st, acc, halves, kbuf, pbuf, ssend, srecv, psend, precv, part, zsend, zrecv,
    ckbuf, cvbuf, cpbuf, cubuf, coef,
    w_sem, big_sem, ag_send, ag_recv, fw_send, fw_recv, ex_send, ex_recv, p_send, p_recv, z_send, z_recv,
):
    kv, tp = lax.axis_index("kv"), lax.axis_index("tp")
    rows, feat = tok_ref.shape
    seqs, cols, width = st.shape
    group = cols // heads
    allheads = wd_ref.shape[0]
    partner = {"tp": 1 - tp}

    def far(d):
        return lax.rem(kv + d, nkv)

    hops = sorted(range(1, nkv), key=lambda d: (min(d, nkv - d), d))
    early, late = hops[:2], hops[2:]
    order = [(0, 0), (0, 1)] + [(d, 0) for d in early]
    order += [(d, 1) for d in early] + [(d, e) for d in late for e in (0, 1)]

    def owner(d, e):
        return far(d) * 2 + (tp if e == 0 else 1 - tp)

    def span(block):
        return pl.ds(pl.multiple_of(block * feat, 128), feat)

    mats = (wq_ref, wk_ref, wv_ref, wg_ref, wd_ref, wb_ref)
    tops = [0, cols, 2 * cols, 3 * cols, 4 * cols, 4 * cols + allheads]
    loads = []
    for n, (d, e) in enumerate(order):
        there = span(owner(d, e))
        chunk = []
        for m, ref in enumerate(mats):
            chunk.append(
                pltpu.make_async_copy(
                    ref.at[:, there], w.at[pl.ds(tops[m], ref.shape[0]), there], w_sem.at[n, m]
                )
            )
        loads.append(chunk)

    barrier = pltpu.get_barrier_semaphore()
    pl.semaphore_signal(barrier, inc=1, device_id=partner, device_id_type=MESH)
    for d in hops:
        pl.semaphore_signal(barrier, inc=1, device_id={"kv": far(d)}, device_id_type=MESH)
    st_copy = pltpu.make_async_copy(st_ref, st, big_sem.at[0])
    wo_copy = pltpu.make_async_copy(wo_ref, wo, big_sem.at[1])
    st_copy.start()
    for chunk in loads:
        for copy in chunk:
            copy.start()
    wo_copy.start()
    pl.semaphore_wait(barrier, nkv)

    def remote(src, dst, send, recv, where):
        return pltpu.make_async_remote_copy(
            src_ref=src, dst_ref=dst, send_sem=send, recv_sem=recv, device_id=where, device_id_type=MESH
        )

    direct, passed = {}, {}
    for d in hops:
        direct[d] = remote(tok_ref, xs.at[d, 0], ag_send.at[d], ag_recv.at[d], {"kv": lax.rem(kv + nkv - d, nkv)})
        direct[d].start()
    passed[0] = remote(tok_ref, xs.at[0, 1], fw_send.at[0], fw_recv.at[0], partner)
    passed[0].start()

    def hand_on(d):
        direct[d].wait_recv()
        passed[d] = remote(xs.at[d, 0], xs.at[d, 1], fw_send.at[d], fw_recv.at[d], partner)
        passed[d].start()

    coefficients(steps, heads, cols, pd_ref, pb_ref, acc_ref, coef)
    st_copy.wait()
    block = 8
    for i in range(seqs // block):
        few = pl.ds(i * block, block)
        held = pl.ds(i * block * steps * heads, block * steps * heads)
        commit_block(
            steps, heads, i, ok_ref.at[held], ov_ref.at[held], st.at[few], com_ref.at[few],
            ckbuf, cvbuf, cpbuf, cubuf, coef,
        )
    for d in early:
        hand_on(d)

    square = jnp.zeros((rows, 1), F32)
    for n, (d, e) in enumerate(order):
        block = owner(d, e)
        if n == 2 + len(early):
            for far_d in late:
                hand_on(far_d)
        if n == 0:
            x = tok_ref[...]
        else:
            if e == 1:
                passed[d].wait_recv()
            x = xs[d, e]
        x = x.astype(F32)
        square = square + jnp.sum(x * x, axis=1, keepdims=True)
        xg = (x * gain_ref[:, span(block)]).astype(BF16)
        for copy in loads[n]:
            copy.wait()
        product = dot_nt(xg, w[:, span(block)])
        if n == 0:
            acc[...] = product
        else:
            acc[...] += product
    scale = lax.rsqrt(square / (feat * nkv * 2) + EPS)

    halves[tp] = (acc[:, : 2 * cols] * scale).astype(BF16)
    qk = remote(halves.at[tp], halves.at[tp], ex_send.at[0], ex_recv.at[0], partner)
    qk.start()
    pending_tail = [qk]

    value = silu((acc[:, 2 * cols : 3 * cols] * scale).astype(BF16).astype(F32))
    gate = silu((acc[:, 3 * cols : 4 * cols] * scale).astype(BF16).astype(F32)) * jnp.concatenate([hg_ref[...]] * heads, axis=1)
    pre = acc[:, 4 * cols :] * scale
    pick_row = lax.broadcasted_iota(jnp.int32, (allheads, cols), 0)
    pick = (pick_row == kv * heads + lane_group(allheads, cols, group)).astype(F32)
    dec = jnp.dot(pre[:, :allheads], pick, precision=lax.Precision.HIGHEST, preferred_element_type=F32)
    bet = jnp.dot(pre[:, allheads:], pick, precision=lax.Precision.HIGHEST, preferred_element_type=F32)
    lanes_own = lane_group(1, cols, group)
    rate = jnp.zeros((1, cols), F32)
    for h in range(heads):
        rate = jnp.where(lanes_own == h, rate_ref[:, h : h + 1], rate)
    soft = jnp.maximum(dec, 0.0) + jnp.log1p(jnp.exp(-jnp.abs(dec)))
    retain = jnp.exp(-(rate * soft))
    strength = jax.nn.sigmoid(bet)
    ones_wide = block_ones(heads * width, width, cols, group)
    ones_cols = block_ones(cols, group, cols, group)

    def at(x, t):
        return x[t * seqs : (t + 1) * seqs]

    remote(halves.at[1 - tp], halves.at[1 - tp], ex_send.at[0], ex_recv.at[0], partner).wait_recv()
    low, high = halves[0].astype(F32), halves[1].astype(F32)
    low, high = silu(low), silu(high)

    def whole(kind):
        base = kind * cols
        pieces = []
        for h in range(heads):
            lanes = slice(base + h * group, base + (h + 1) * group)
            pieces += [low[:, lanes], high[:, lanes]]
        return jnp.concatenate(pieces, axis=1)

    query, key = whole(0), whole(1)
    for t in range(steps):
        for h in range(heads):
            lanes = slice(h * width, (h + 1) * width)
            place = (h * 2) * steps + t
            kbuf[pl.ds(place, seqs, stride=heads * 2 * steps), :] = at(key, t)[:, lanes]
            kbuf[pl.ds(place + steps, seqs, stride=heads * 2 * steps), :] = at(query, t)[:, lanes]
    tall = 2 * steps
    for s in range(seqs):
        stacked = kbuf[pl.ds(s * heads * tall, heads * tall), :].astype(BF16)
        seen = dot_nt(stacked, com_ref[s].astype(BF16))
        put(
            pbuf,
            pl.ds(s * tall, tall),
            own_head([seen[h * tall : (h + 1) * tall] for h in range(heads)], group),
        )
    pairs = [("k", i, t) for t in range(steps) for i in range(t + 1)]
    pairs += [("q", i, t) for t in range(steps) for i in range(t + 1)]
    products = [at(key, i) * at(key if kind == "k" else query, t) for kind, i, t in pairs]
    products.append(query * query)
    sums = jnp.dot(
        jnp.concatenate(products, axis=0).astype(BF16), ones_wide, preferred_element_type=F32
    )
    gram = {pair: at(sums, n) for n, pair in enumerate(pairs)}
    qsq = sums[len(pairs) * seqs :]
    qnorm = lax.rsqrt(qsq + EPS) * width ** (-0.5)
    fed, through, outs = [], None, []
    for t in range(steps):
        norm = lax.rsqrt(gram[("k", t, t)] + EPS)
        a = at(retain, t)
        through = a if through is None else through * a
        fed = [a * f for f in fed]
        predicted = through * get(pbuf, pl.ds(t, seqs, stride=tall), cols)
        for i in range(t):
            predicted = predicted + gram[("k", i, t)] * fed[i]
        fed.append(at(strength, t) * (at(value, t) - norm * predicted) * norm)
        o = through * get(pbuf, pl.ds(steps + t, seqs, stride=tall), cols)
        for i in range(t + 1):
            o = o + gram[("q", i, t)] * fed[i]
        outs.append(o * at(qnorm, t))
    heads_out = jnp.concatenate(outs, axis=0)
    squares = jnp.dot((heads_out * heads_out).astype(BF16), ones_cols, preferred_element_type=F32)
    ssend[...] = squares
    sq = remote(ssend, srecv, ex_send.at[1], ex_recv.at[1], partner)
    sq.start()
    ready = heads_out * gate
    wo_copy.wait()
    sq.wait_recv()
    pending_tail.append(sq)
    total = squares + srecv[...]
    scaled = (ready * lax.rsqrt(total / (2 * group) + EPS)).astype(BF16)

    targets = sorted(range(1, nkv), key=lambda d: (-min(d, nkv - d), d)) + [0]
    crossing = []
    for j, d in enumerate(targets):
        psend[j] = jnp.dot(scaled, wo[:, span(owner(d, 1))], preferred_element_type=F32).astype(BF16)
        copy = remote(psend.at[j], precv.at[j], p_send.at[j], p_recv.at[j], partner)
        copy.start()
        crossing.append(copy)
        part[j] = jnp.dot(scaled, wo[:, span(owner(d, 0))], preferred_element_type=F32)
    flights = []
    for j, d in enumerate(targets):
        crossing[j].wait_recv()
        both = part[j] + precv[j].astype(F32)
        if d:
            zsend[j] = both.astype(BF16)
            copy = remote(zsend.at[j], zrecv.at[j], z_send.at[j], z_recv.at[j], {"kv": far(d)})
            copy.start()
            flights.append(copy)
    mixed = both
    for j, copy in sorted(enumerate(flights), key=lambda f: -f[0]):
        copy.wait_recv()
        mixed = mixed + zrecv[j].astype(F32)
    out_ref[...] = mixed.astype(BF16)
    for copy in [*direct.values(), *passed.values()] + pending_tail + crossing + flights:
        copy.wait_send()


def local(
    nkv,
    tokens,
    norm_gain,
    w_query,
    w_key,
    w_value,
    w_gate,
    w_decay,
    w_beta,
    decay_rate,
    head_gain,
    w_out,
    state,
    prev_keys,
    prev_values,
    prev_decay,
    prev_beta,
    accepted,
):
    seqs, steps, feat = tokens.shape
    heads, group, width = state.shape[1:]
    cols = heads * group
    rows = seqs * steps
    full = norm_gain.shape[0]
    allheads = w_decay.shape[1]
    vmem = pl.BlockSpec(memory_space=pltpu.VMEM)
    hbm = pl.BlockSpec(memory_space=pltpu.HBM)
    tiles = pl.cdiv(cols, 128)
    old = 8 * steps * heads
    blocks = 2 * nkv
    tall = 2 * steps
    DMA = pltpu.SemaphoreType.DMA
    mixed, committed = pl.pallas_call(
        functools.partial(verify_kernel, nkv, heads, steps),
        out_shape=(
            jax.ShapeDtypeStruct((rows, feat), BF16),
            pltpu.VMEM((seqs, cols, width), F32),
        ),
        in_specs=[vmem] * 2 + [hbm] * 6 + [vmem, vmem] + [hbm] * 2 + [vmem] * 5,
        out_specs=(vmem, vmem),
        scratch_shapes=[
            pltpu.VMEM((nkv, 2, rows, feat), BF16),
            pltpu.VMEM((4 * cols + 2 * allheads, full), BF16),
            pltpu.VMEM((cols, full), BF16),
            pltpu.VMEM((seqs, cols, width), F32),
            pltpu.VMEM((rows, 4 * cols + 2 * allheads), F32),
            pltpu.VMEM((2, rows, 2 * cols), BF16),
            pltpu.VMEM((seqs * heads * tall, width), F32),
            pltpu.VMEM((pl.cdiv(cols, 128), seqs * tall, 128), F32),
            pltpu.VMEM((rows, cols), F32),
            pltpu.VMEM((rows, cols), F32),
            pltpu.VMEM((nkv, rows, feat), BF16),
            pltpu.VMEM((nkv, rows, feat), BF16),
            pltpu.VMEM((nkv, rows, feat), F32),
            pltpu.VMEM((nkv, rows, feat), BF16),
            pltpu.VMEM((nkv, rows, feat), BF16),
            pltpu.VMEM((old, width), F32),
            pltpu.VMEM((old, width), F32),
            pltpu.VMEM((tiles, old, 128), F32),
            pltpu.VMEM((tiles, old, 128), F32),
            pltpu.VMEM((2 * steps, seqs, cols), F32),
            DMA((blocks, 6)),
            DMA((2,)),
            DMA((nkv,)),
            DMA((nkv,)),
            DMA((nkv,)),
            DMA((nkv,)),
            DMA((2,)),
            DMA((2,)),
            DMA((nkv,)),
            DMA((nkv,)),
            DMA((nkv,)),
            DMA((nkv,)),
        ],
        compiler_params=pltpu.CompilerParams(
            collective_id=0, has_side_effects=True, vmem_limit_bytes=57 * 1024 * 1024
        ),
    )(
        jnp.transpose(tokens, (1, 0, 2)).reshape(rows, feat),
        norm_gain.reshape(1, full),
        w_query.reshape(cols, full),
        w_key.reshape(cols, full),
        w_value.reshape(cols, full),
        w_gate.reshape(cols, full),
        w_decay.T,
        w_beta.T,
        decay_rate.reshape(1, heads),
        head_gain.reshape(1, group),
        w_out.reshape(cols, full),
        state.reshape(seqs, cols, width),
        prev_keys.reshape(seqs * steps * heads, width),
        prev_values.reshape(seqs * steps * heads, group),
        jnp.transpose(prev_decay, (1, 2, 0)).reshape(steps * heads, seqs),
        jnp.transpose(prev_beta, (1, 2, 0)).reshape(steps * heads, seqs),
        accepted.reshape(1, seqs),
    )
    mixed = jnp.transpose(mixed.reshape(steps, seqs, feat), (1, 0, 2))
    return mixed, committed.reshape(state.shape)


def solution(mesh):
    in_specs = (
        P(("grp", "dp"), None, ("kv", "tp")),
        P(),
        P("kv", "tp", None),
        P("kv", "tp", None),
        P("kv", "tp", None),
        P("kv", "tp", None),
        P(),
        P(),
        P("kv"),
        P("tp"),
        P("kv", "tp", None),
        P(("grp", "dp"), "kv", "tp", None),
        P(("grp", "dp"), None, "kv", None),
        P(("grp", "dp"), None, "kv", "tp"),
        P(("grp", "dp"), None, "kv"),
        P(("grp", "dp"), None, "kv"),
        P(("grp", "dp")),
    )
    out_specs = (P(("grp", "dp"), None, ("kv", "tp")), P(("grp", "dp"), "kv", "tp", None))
    return jax.shard_map(
        functools.partial(local, mesh.shape["kv"]),
        mesh=mesh, in_specs=in_specs, out_specs=out_specs, check_vma=False,
    )
```

```python
import functools

import jax
import jax.numpy as jnp
from jax import lax
from jax.experimental import pallas as pl
from jax.experimental.pallas import tpu as pltpu
from jax.sharding import PartitionSpec as P

EPS = 1e-06
F32 = jnp.float32
BF16 = jnp.bfloat16
MESH = pl.DeviceIdType.MESH
NT = (((1,), (1,)), ((), ()))
TN = (((0,), (0,)), ((), ()))


def dot_nt(a, b):
    return lax.dot_general(a, b, NT, preferred_element_type=F32)


def silu(u):
    return u * jax.nn.sigmoid(u)


def lane_group(rows, cols, group):
    return lax.broadcasted_iota(jnp.int32, (rows, cols), 1) // group


def block_ones(rows, row_group, cols, col_group):
    r = lax.broadcasted_iota(jnp.int32, (rows, cols), 0) // row_group
    return (r == lane_group(rows, cols, col_group)).astype(F32).astype(BF16)


def put(buf, rows, x):
    cols = x.shape[1]
    if cols < 128:
        x = jnp.concatenate([x] * (128 // cols), axis=1)
    for c in range(buf.shape[0]):
        buf[c, rows, :] = x[:, c * 128 : (c + 1) * 128]


def get(buf, rows, cols):
    x = jnp.concatenate([buf[c, rows, :] for c in range(buf.shape[0])], axis=1)
    return x[:, :cols]


def own_head(parts, group):
    rows, cols = parts[0].shape
    if len(parts) == 1:
        return parts[0]
    lanes = lane_group(rows, cols, group)
    total = jnp.where(lanes == 0, parts[0], 0.0)
    for h in range(1, len(parts)):
        total = jnp.where(lanes == h, parts[h], total)
    return total


def coefficients(steps, heads, cols, pd_ref, pb_ref, acc_ref, coef):
    rows = steps * heads
    group = cols // heads
    total = acc_ref.shape[1]
    step_of = lax.broadcasted_iota(jnp.int32, (rows, total), 0) // heads
    mask = (step_of < acc_ref[...]).astype(F32)
    retain = jnp.exp(-pd_ref[...] * mask)
    beta = pb_ref[...] * mask
    head_of = lax.broadcasted_iota(jnp.int32, (rows, cols), 0)
    for t in range(steps):
        pick = (head_of == t * heads + lane_group(rows, cols, group)).astype(F32)
        for n, x in enumerate((retain, beta)):
            coef[n * steps + t] = lax.dot_general(
                x, pick, TN, precision=lax.Precision.HIGHEST, preferred_element_type=F32
            )


def commit_block(steps, heads, block, k_ref, v_ref, s_ref, out_ref, kbuf, vbuf, pbuf, ubuf, coef):
    seqs, cols, width = s_ref.shape
    group = cols // heads
    rows = steps * heads
    kbuf[...] = k_ref[...].astype(F32)
    values = v_ref[...].astype(F32)
    vbuf[...] = jnp.concatenate([values] * (width // group), axis=1)
    for s in range(seqs):
        put(
            pbuf,
            pl.ds(s * rows, rows),
            dot_nt(k_ref[pl.ds(s * rows, rows), :], s_ref[s].astype(BF16)),
        )

    def every(t, h):
        return pl.ds(t * heads + h, seqs, stride=rows)

    keys = [[kbuf[every(t, h), :] for h in range(heads)] for t in range(steps)]
    pairs = [(i, t) for t in range(steps) for i in range(t + 1)]
    products = [
        jnp.concatenate([keys[i][h] * keys[t][h] for h in range(heads)], axis=1) for i, t in pairs
    ]
    sums = jnp.dot(
        jnp.concatenate(products, axis=0).astype(BF16),
        block_ones(heads * width, width, cols, group),
        preferred_element_type=F32,
    )
    gram = {pair: sums[n * seqs : (n + 1) * seqs] for n, pair in enumerate(pairs)}
    norm = [lax.rsqrt(gram[(t, t)] + EPS) for t in range(steps)]
    here = pl.ds(block * seqs, seqs)
    fed = []
    through = None
    copies = max(1, cols // width)
    for t in range(steps):
        decay = coef[t, here, :]
        seen = own_head([get(pbuf, every(t, h), cols) for h in range(heads)], group)
        value = own_head(
            [jnp.concatenate([vbuf[every(t, h), :]] * copies, axis=1)[:, :cols] for h in range(heads)],
            group,
        )
        through = decay if through is None else through * decay
        fed = [decay * f for f in fed]
        predicted = through * seen
        for i in range(t):
            predicted = predicted + gram[(i, t)] * fed[i]
        fed.append(coef[steps + t, here, :] * (value - norm[t] * predicted) * norm[t])
    lanes = lane_group(seqs, cols, group)
    for t in range(steps):
        for h in range(heads):
            put(ubuf, every(t, h), jnp.where(lanes == h, fed[t], 0.0))
    for s in range(seqs):
        update = lax.dot_general(
            get(ubuf, pl.ds(s * rows, rows), cols).astype(BF16),
            k_ref[pl.ds(s * rows, rows), :],
            TN,
            preferred_element_type=F32,
        )
        for h in range(heads):
            span = slice(h * group, (h + 1) * group)
            kept = through[s : s + 1, h * group : h * group + 1]
            out_ref[s, span, :] = kept * s_ref[s, span, :] + update[span]


def verify_kernel(
    nkv, heads, steps,
    tok_ref, gain_ref, wq_ref, wk_ref, wv_ref, wg_ref, wd_ref, wb_ref, rate_ref, hg_ref, wo_ref, st_ref,
    ok_ref, ov_ref, pd_ref, pb_ref, acc_ref,
    out_ref, com_ref,
    xs, w, wo, st, acc, halves, kbuf, pbuf, ssend, srecv, psend, precv, part, zsend, zrecv,
    ckbuf, cvbuf, cpbuf, cubuf, coef,
    w_sem, big_sem, ag_send, ag_recv, fw_send, fw_recv, ex_send, ex_recv, p_send, p_recv, z_send, z_recv,
):
    kv, tp = lax.axis_index("kv"), lax.axis_index("tp")
    rows, feat = tok_ref.shape
    seqs, cols, width = st.shape
    group = cols // heads
    allheads = wd_ref.shape[0]
    partner = {"tp": 1 - tp}

    def far(d):
        return lax.rem(kv + d, nkv)

    hops = sorted(range(1, nkv), key=lambda d: (min(d, nkv - d), d))
    early, late = hops[:2], hops[2:]
    order = [(0, 0), (0, 1)] + [(d, 0) for d in early]
    order += [(d, 1) for d in early] + [(d, e) for d in late for e in (0, 1)]

    def owner(d, e):
        return far(d) * 2 + (tp if e == 0 else 1 - tp)

    def span(block):
        return pl.ds(pl.multiple_of(block * feat, 128), feat)

    mats = (wq_ref, wk_ref, wv_ref, wg_ref, wd_ref, wb_ref)
    tops = [0, cols, 2 * cols, 3 * cols, 4 * cols, 4 * cols + allheads]
    loads = []
    for n, (d, e) in enumerate(order):
        there = span(owner(d, e))
        chunk = []
        for m, ref in enumerate(mats):
            chunk.append(
                pltpu.make_async_copy(
                    ref.at[:, there], w.at[pl.ds(tops[m], ref.shape[0]), there], w_sem.at[n, m]
                )
            )
        loads.append(chunk)

    barrier = pltpu.get_barrier_semaphore()
    pl.semaphore_signal(barrier, inc=1, device_id=partner, device_id_type=MESH)
    for d in hops:
        pl.semaphore_signal(barrier, inc=1, device_id={"kv": far(d)}, device_id_type=MESH)
    st_copy = pltpu.make_async_copy(st_ref, st, big_sem.at[0])
    wo_copy = pltpu.make_async_copy(wo_ref, wo, big_sem.at[1])
    st_copy.start()
    for chunk in loads:
        for copy in chunk:
            copy.start()
    wo_copy.start()
    pl.semaphore_wait(barrier, nkv)

    def remote(src, dst, send, recv, where):
        return pltpu.make_async_remote_copy(
            src_ref=src, dst_ref=dst, send_sem=send, recv_sem=recv, device_id=where, device_id_type=MESH
        )

    direct, passed = {}, {}
    for d in hops:
        direct[d] = remote(tok_ref, xs.at[d, 0], ag_send.at[d], ag_recv.at[d], {"kv": lax.rem(kv + nkv - d, nkv)})
        direct[d].start()
    passed[0] = remote(tok_ref, xs.at[0, 1], fw_send.at[0], fw_recv.at[0], partner)
    passed[0].start()

    def hand_on(d):
        direct[d].wait_recv()
        passed[d] = remote(xs.at[d, 0], xs.at[d, 1], fw_send.at[d], fw_recv.at[d], partner)
        passed[d].start()

    coefficients(steps, heads, cols, pd_ref, pb_ref, acc_ref, coef)
    st_copy.wait()
    block = 8
    for i in range(seqs // block):
        few = pl.ds(i * block, block)
        held = pl.ds(i * block * steps * heads, block * steps * heads)
        commit_block(
            steps, heads, i, ok_ref.at[held], ov_ref.at[held], st.at[few], com_ref.at[few],
            ckbuf, cvbuf, cpbuf, cubuf, coef,
        )
    for d in early:
        hand_on(d)

    square = jnp.zeros((rows, 1), F32)
    for n, (d, e) in enumerate(order):
        block = owner(d, e)
        if n == 2 + len(early):
            for far_d in late:
                hand_on(far_d)
        if n == 0:
            x = tok_ref[...]
        else:
            if e == 1:
                passed[d].wait_recv()
            x = xs[d, e]
        x = x.astype(F32)
        square = square + jnp.sum(x * x, axis=1, keepdims=True)
        xg = (x * gain_ref[:, span(block)]).astype(BF16)
        for copy in loads[n]:
            copy.wait()
        product = dot_nt(xg, w[:, span(block)])
        if n == 0:
            acc[...] = product
        else:
            acc[...] += product
    scale = lax.rsqrt(square / (feat * nkv * 2) + EPS)

    halves[tp] = (acc[:, : 2 * cols] * scale).astype(BF16)
    qk = remote(halves.at[tp], halves.at[tp], ex_send.at[0], ex_recv.at[0], partner)
    qk.start()
    pending_tail = [qk]

    value = silu((acc[:, 2 * cols : 3 * cols] * scale).astype(BF16).astype(F32))
    gate = silu((acc[:, 3 * cols : 4 * cols] * scale).astype(BF16).astype(F32)) * jnp.concatenate([hg_ref[...]] * heads, axis=1)
    pre = acc[:, 4 * cols :] * scale
    pick_row = lax.broadcasted_iota(jnp.int32, (allheads, cols), 0)
    pick = (pick_row == kv * heads + lane_group(allheads, cols, group)).astype(F32)
    dec = jnp.dot(pre[:, :allheads], pick, precision=lax.Precision.HIGHEST, preferred_element_type=F32)
    bet = jnp.dot(pre[:, allheads:], pick, precision=lax.Precision.HIGHEST, preferred_element_type=F32)
    lanes_own = lane_group(1, cols, group)
    rate = jnp.zeros((1, cols), F32)
    for h in range(heads):
        rate = jnp.where(lanes_own == h, rate_ref[:, h : h + 1], rate)
    soft = jnp.maximum(dec, 0.0) + jnp.log1p(jnp.exp(-jnp.abs(dec)))
    retain = jnp.exp(-(rate * soft))
    strength = jax.nn.sigmoid(bet)
    ones_wide = block_ones(heads * width, width, cols, group)
    ones_cols = block_ones(cols, group, cols, group)

    def at(x, t):
        return x[t * seqs : (t + 1) * seqs]

    remote(halves.at[1 - tp], halves.at[1 - tp], ex_send.at[0], ex_recv.at[0], partner).wait_recv()
    low, high = halves[0].astype(F32), halves[1].astype(F32)
    low, high = silu(low), silu(high)

    def whole(kind):
        base = kind * cols
        pieces = []
        for h in range(heads):
            lanes = slice(base + h * group, base + (h + 1) * group)
            pieces += [low[:, lanes], high[:, lanes]]
        return jnp.concatenate(pieces, axis=1)

    query, key = whole(0), whole(1)
    for t in range(steps):
        for h in range(heads):
            lanes = slice(h * width, (h + 1) * width)
            place = (h * 2) * steps + t
            kbuf[pl.ds(place, seqs, stride=heads * 2 * steps), :] = at(key, t)[:, lanes]
            kbuf[pl.ds(place + steps, seqs, stride=heads * 2 * steps), :] = at(query, t)[:, lanes]
    tall = 2 * steps
    for s in range(seqs):
        stacked = kbuf[pl.ds(s * heads * tall, heads * tall), :].astype(BF16)
        seen = dot_nt(stacked, com_ref[s].astype(BF16))
        put(
            pbuf,
            pl.ds(s * tall, tall),
            own_head([seen[h * tall : (h + 1) * tall] for h in range(heads)], group),
        )
    pairs = [("k", i, t) for t in range(steps) for i in range(t + 1)]
    pairs += [("q", i, t) for t in range(steps) for i in range(t + 1)]
    products = [at(key, i) * at(key if kind == "k" else query, t) for kind, i, t in pairs]
    products.append(query * query)
    sums = jnp.dot(
        jnp.concatenate(products, axis=0).astype(BF16), ones_wide, preferred_element_type=F32
    )
    gram = {pair: at(sums, n) for n, pair in enumerate(pairs)}
    qsq = sums[len(pairs) * seqs :]
    qnorm = lax.rsqrt(qsq + EPS) * width ** (-0.5)
    fed, through, outs = [], None, []
    for t in range(steps):
        norm = lax.rsqrt(gram[("k", t, t)] + EPS)
        a = at(retain, t)
        through = a if through is None else through * a
        fed = [a * f for f in fed]
        predicted = through * get(pbuf, pl.ds(t, seqs, stride=tall), cols)
        for i in range(t):
            predicted = predicted + gram[("k", i, t)] * fed[i]
        fed.append(at(strength, t) * (at(value, t) - norm * predicted) * norm)
        o = through * get(pbuf, pl.ds(steps + t, seqs, stride=tall), cols)
        for i in range(t + 1):
            o = o + gram[("q", i, t)] * fed[i]
        outs.append(o * at(qnorm, t))
    heads_out = jnp.concatenate(outs, axis=0)
    squares = jnp.dot((heads_out * heads_out).astype(BF16), ones_cols, preferred_element_type=F32)
    ssend[...] = squares
    sq = remote(ssend, srecv, ex_send.at[1], ex_recv.at[1], partner)
    sq.start()
    ready = heads_out * gate
    wo_copy.wait()
    sq.wait_recv()
    pending_tail.append(sq)
    total = squares + srecv[...]
    scaled = (ready * lax.rsqrt(total / (2 * group) + EPS)).astype(BF16)

    targets = sorted(range(1, nkv), key=lambda d: (-min(d, nkv - d), d)) + [0]
    crossing, flights = [], []

    def chip_sum(j):
        crossing[j].wait_recv()
        both = part[j] + precv[j].astype(F32)
        if targets[j]:
            zsend[j] = both.astype(BF16)
            copy = remote(zsend.at[j], zrecv.at[j], z_send.at[j], z_recv.at[j], {"kv": far(targets[j])})
            copy.start()
            flights.append(copy)
        return both

    for j, d in enumerate(targets):
        psend[j] = jnp.dot(scaled, wo[:, span(owner(d, 1))], preferred_element_type=F32).astype(BF16)
        copy = remote(psend.at[j], precv.at[j], p_send.at[j], p_recv.at[j], partner)
        copy.start()
        crossing.append(copy)
        part[j] = jnp.dot(scaled, wo[:, span(owner(d, 0))], preferred_element_type=F32)
        if j >= 2:
            chip_sum(j - 2)
    for j in range(max(0, nkv - 2), nkv):
        both = chip_sum(j)
    mixed = both
    for j, copy in sorted(enumerate(flights), key=lambda f: -f[0]):
        copy.wait_recv()
        mixed = mixed + zrecv[j].astype(F32)
    out_ref[...] = mixed.astype(BF16)
    for copy in [*direct.values(), *passed.values()] + pending_tail + crossing + flights:
        copy.wait_send()


def local(
    nkv,
    tokens,
    norm_gain,
    w_query,
    w_key,
    w_value,
    w_gate,
    w_decay,
    w_beta,
    decay_rate,
    head_gain,
    w_out,
    state,
    prev_keys,
    prev_values,
    prev_decay,
    prev_beta,
    accepted,
):
    seqs, steps, feat = tokens.shape
    heads, group, width = state.shape[1:]
    cols = heads * group
    rows = seqs * steps
    full = norm_gain.shape[0]
    allheads = w_decay.shape[1]
    vmem = pl.BlockSpec(memory_space=pltpu.VMEM)
    hbm = pl.BlockSpec(memory_space=pltpu.HBM)
    tiles = pl.cdiv(cols, 128)
    old = 8 * steps * heads
    blocks = 2 * nkv
    tall = 2 * steps
    DMA = pltpu.SemaphoreType.DMA
    mixed, committed = pl.pallas_call(
        functools.partial(verify_kernel, nkv, heads, steps),
        out_shape=(
            pltpu.VMEM((rows, feat), BF16),
            pltpu.VMEM((seqs, cols, width), F32),
        ),
        in_specs=[vmem] * 2 + [hbm] * 6 + [vmem, vmem] + [hbm] * 2 + [vmem] * 5,
        out_specs=(vmem, vmem),
        scratch_shapes=[
            pltpu.VMEM((nkv, 2, rows, feat), BF16),
            pltpu.VMEM((4 * cols + 2 * allheads, full), BF16),
            pltpu.VMEM((cols, full), BF16),
            pltpu.VMEM((seqs, cols, width), F32),
            pltpu.VMEM((rows, 4 * cols + 2 * allheads), F32),
            pltpu.VMEM((2, rows, 2 * cols), BF16),
            pltpu.VMEM((seqs * heads * tall, width), F32),
            pltpu.VMEM((pl.cdiv(cols, 128), seqs * tall, 128), F32),
            pltpu.VMEM((rows, cols), F32),
            pltpu.VMEM((rows, cols), F32),
            pltpu.VMEM((nkv, rows, feat), BF16),
            pltpu.VMEM((nkv, rows, feat), BF16),
            pltpu.VMEM((nkv, rows, feat), F32),
            pltpu.VMEM((nkv, rows, feat), BF16),
            pltpu.VMEM((nkv, rows, feat), BF16),
            pltpu.VMEM((old, width), F32),
            pltpu.VMEM((old, width), F32),
            pltpu.VMEM((tiles, old, 128), F32),
            pltpu.VMEM((tiles, old, 128), F32),
            pltpu.VMEM((2 * steps, seqs, cols), F32),
            DMA((blocks, 6)),
            DMA((2,)),
            DMA((nkv,)),
            DMA((nkv,)),
            DMA((nkv,)),
            DMA((nkv,)),
            DMA((2,)),
            DMA((2,)),
            DMA((nkv,)),
            DMA((nkv,)),
            DMA((nkv,)),
            DMA((nkv,)),
        ],
        compiler_params=pltpu.CompilerParams(
            collective_id=0, has_side_effects=True, vmem_limit_bytes=57 * 1024 * 1024
        ),
    )(
        pltpu.with_memory_space_constraint(
            jnp.transpose(tokens, (1, 0, 2)).reshape(rows, feat), pltpu.VMEM
        ),
        norm_gain.reshape(1, full),
        w_query.reshape(cols, full),
        w_key.reshape(cols, full),
        w_value.reshape(cols, full),
        w_gate.reshape(cols, full),
        w_decay.T,
        w_beta.T,
        decay_rate.reshape(1, heads),
        head_gain.reshape(1, group),
        w_out.reshape(cols, full),
        state.reshape(seqs, cols, width),
        prev_keys.reshape(seqs * steps * heads, width),
        prev_values.reshape(seqs * steps * heads, group),
        jnp.transpose(prev_decay, (1, 2, 0)).reshape(steps * heads, seqs),
        jnp.transpose(prev_beta, (1, 2, 0)).reshape(steps * heads, seqs),
        accepted.reshape(1, seqs),
    )
    mixed = jnp.transpose(mixed.reshape(steps, seqs, feat), (1, 0, 2))
    return mixed, committed.reshape(state.shape)


def solution(mesh):
    in_specs = (
        P(("grp", "dp"), None, ("kv", "tp")),
        P(),
        P("kv", "tp", None),
        P("kv", "tp", None),
        P("kv", "tp", None),
        P("kv", "tp", None),
        P(),
        P(),
        P("kv"),
        P("tp"),
        P("kv", "tp", None),
        P(("grp", "dp"), "kv", "tp", None),
        P(("grp", "dp"), None, "kv", None),
        P(("grp", "dp"), None, "kv", "tp"),
        P(("grp", "dp"), None, "kv"),
        P(("grp", "dp"), None, "kv"),
        P(("grp", "dp")),
    )
    out_specs = (P(("grp", "dp"), None, ("kv", "tp")), P(("grp", "dp"), "kv", "tp", None))
    return jax.shard_map(
        functools.partial(local, mesh.shape["kv"]),
        mesh=mesh, in_specs=in_specs, out_specs=out_specs, check_vma=False,
    )
```
